32 devices in a mesh: dp: 4 (over y, x), kv: 4 (over z), tp: 2 (over core).
Axes of the slice: x: 2, y: 2, z: 4, core: 2. Of those that a mesh axis runs over, the one named last changes fastest.
Arguments:
- tokens: bfloat16 [96, 4096], P('dp', ('kv', 'tp')), may hold values from -10 to 10
- gain_mixer: bfloat16 [4096], replicated, may hold values from 0.099609375 to 1.8984375
- weight_query: bfloat16 [4096, 16, 128], P('kv', 'tp'), may hold values from -0.09375 to 0.09375
- weight_key: bfloat16 [4096, 16, 128], P('kv', 'tp'), may hold values from -0.09375 to 0.09375
- weight_value: bfloat16 [4096, 16, 128], P('kv', 'tp'), may hold values from -0.09375 to 0.09375
- weight_outgate: bfloat16 [4096, 16, 128], P('kv', 'tp'), may hold values from -0.09375 to 0.09375
- weight_ingate: bfloat16 [4096, 16], replicated, may hold values from -0.09375 to 0.09375
- weight_forget: bfloat16 [4096, 16], replicated, may hold values from -0.09375 to 0.09375
- bias_input: float32 [16], replicated, may hold values from -3 to 3
- bias_forget: float32 [16], replicated, may hold values from 0 to 5
- memory: float32 [96, 16, 128, 128], P(('dp', 'kv'), 'tp'), may hold values from -2.5 to 2.5
- normalizer: float32 [96, 16, 128], P(('dp', 'kv'), 'tp'), may hold values from -2.5 to 2.5
- stabilizer: float32 [96, 16], P(('dp', 'kv'), 'tp'), may hold values from -1 to 3
- head_gain: bfloat16 [16, 128], replicated, may hold values from 0.099609375 to 1.8984375
- weight_out: bfloat16 [2048, 4096], P('tp', 'kv'), may hold values from -0.125 to 0.125
- gain_channel: bfloat16 [4096], replicated, may hold values from 0.099609375 to 1.8984375
- weight_up: bfloat16 [4096, 16384], P(None, ('kv', 'tp')), may hold values from -0.09375 to 0.09375
- weight_down: bfloat16 [16384, 4096], P(('kv', 'tp')), may hold values from -0.0625 to 0.0625
Outputs:
- layer_out: bfloat16 [96, 4096], P('dp', ('kv', 'tp'))
- new_memory: float32 [96, 16, 128, 128], P(('dp', 'kv'), 'tp')
- new_normalizer: float32 [96, 16, 128], P(('dp', 'kv'), 'tp')
- new_stabilizer: float32 [96, 16], P(('dp', 'kv'), 'tp')
The draws below stay inside these ranges and needn't reach their ends.
All inputs are finite; a program needn't handle non-finite values.
Results may differ from the reference program's by a relative error of at most 0.017.
Values may be sent and summed in bfloat16 or wider, within the bound.
No kernel may reach another device: no remote copies, remote signals or barrier semaphores. Data moves between devices by JAX's collectives and lax.ppermute only.
A program may use at most 128 MiB of HBM per device.

```python
import math
import jax
import jax.numpy as jnp
from jax import lax

D = 4096
HEADS = 16
HD = 128
WIDTH = 2048
FF = 16384
SEQ_DEV = 6
BATCH = 96
N_DP = 4
N_KV = 4
N_TP = 2


def draw_tokens(key, part):
    columns = jnp.arange(D, dtype=jnp.float32) / (D - 1)
    base = jnp.clip(jax.random.normal(key, (BATCH, D), jnp.float32), -4.0, 4.0)
    rising = jnp.exp(columns * math.log(5.0))
    return (base * rising * 0.5).astype(jnp.bfloat16)


def with_spikes(values, rng, source, target, shards_of, factor):
    def block_of(position):
        return (jnp.arange(values.shape[position]) // (values.shape[position] // shards_of)).reshape((-1,) + (1,) * (values.ndim - 1 - position))

    first = jax.random.permutation(rng, shards_of)[block_of(target)]
    far = (block_of(target) + shards_of // 2) % shards_of
    return jnp.where((block_of(source) == first) | (block_of(source) == far), factor * values, values)


def steps_of(own_key, shape, pieces, low, largest):
    def one(position, parts):
        draws = jax.random.uniform(jax.random.fold_in(jax.random.fold_in(own_key, 6), position), (parts,), jnp.float32, low / len(pieces), largest / len(pieces))
        return jnp.repeat(jnp.exp(draws), shape[position] // parts).reshape((-1,) + (1,) * (len(shape) - position - 1))

    factor_of = one(*pieces[0])
    for cut in pieces[1:]:
        factor_of = factor_of * one(*cut)
    return factor_of


def noise(rng, dims, width, limit, split=(), kind=jnp.bfloat16):
    drawn = width * jax.random.normal(rng, dims, jnp.float32)
    if split:
        drawn = drawn * steps_of(rng, dims, split, -0.22, 0.18)
    return jnp.clip(drawn, -limit, limit).astype(kind)


def noise_with(key, dims, width, most, pieces, heavy, held_as=jnp.bfloat16):
    result = width * jax.random.normal(key, dims, jnp.float32)
    if pieces:
        result = result * steps_of(key, dims, pieces, -0.22, 0.18)
    return jnp.clip(with_spikes(result, jax.random.fold_in(key, 3), *heavy), -most, most).astype(held_as)


def setup_inputs(seed: int = 0) -> dict:
    key_list = jax.random.split(jax.random.key(seed), 19)
    return {
        "tokens": draw_tokens(jax.random.fold_in(key_list[18], 71), 0),
        "gain_mixer": jnp.clip(1.0 + 0.18 * jax.random.normal(key_list[1], (D,), jnp.float32), 0.099609375, 1.8984375).astype(jnp.bfloat16),
        "weight_query": noise(key_list[2], (D, HEADS, HD), D ** -0.5, 0.09375, ((0, 4), (1, 2))),
        "weight_key": noise(key_list[3], (D, HEADS, HD), D ** -0.5, 0.09375, ((0, 4), (1, 2))),
        "weight_value": noise(key_list[4], (D, HEADS, HD), D ** -0.5, 0.09375, ((0, 4), (1, 2))),
        "weight_outgate": noise(key_list[5], (D, HEADS, HD), D ** -0.5, 0.09375, ((0, 4), (1, 2))),
        "weight_ingate": noise(key_list[6], (D, HEADS), D ** -0.5, 0.09375),
        "weight_forget": noise(key_list[7], (D, HEADS), D ** -0.5, 0.09375),
        "bias_input": noise(key_list[8], (HEADS,), 1.0, 3.0, (), jnp.float32),
        "bias_forget": jnp.clip(jax.random.uniform(key_list[9], (HEADS,), jnp.float32, 0.0, 5.0), 0.0, 5.0),
        "memory": noise(key_list[10], (BATCH, HEADS, HD, HD), 0.3, 2.5, ((0, 16), (1, 2)), jnp.float32),
        "normalizer": noise(key_list[11], (BATCH, HEADS, HD), 0.3, 2.5, ((0, 16), (1, 2)), jnp.float32),
        "stabilizer": jnp.clip(-1.0 + 4.0 * jax.random.uniform(key_list[12], (BATCH, HEADS), jnp.float32) ** steps_of(key_list[12], (BATCH, HEADS), ((0, 16), (1, 2)), -0.2, 0.2), -1.0, 3.0),
        "head_gain": jnp.clip(1.0 + 0.18 * jax.random.normal(key_list[13], (HEADS, HD), jnp.float32), 0.099609375, 1.8984375).astype(jnp.bfloat16),
        "weight_out": noise(key_list[14], (WIDTH, D), WIDTH ** -0.5, 0.125, ((0, 2), (1, 4))),
        "gain_channel": jnp.clip(1.0 + 0.18 * jax.random.normal(key_list[15], (D,), jnp.float32), 0.099609375, 1.8984375).astype(jnp.bfloat16),
        "weight_up": noise(key_list[16], (D, FF), D ** -0.5, 0.09375, ((1, 8),)),
        "weight_down": noise_with(key_list[17], (FF, D), FF ** -0.5, 0.0625, ((0, 8),), (0, 1, 8, 2.0)),
    }


epsilon = 1e-06

def project(scaled, weight):
    return jnp.dot(scaled, weight.reshape(weight.shape[0], -1), preferred_element_type=jnp.float32)

def cell_update(queries, keys_in, values_in, outgates, ingate, forget, memory, normalizer, stabilizer, head_scale):
    head_dim = queries.shape[-1]
    query_wide = queries.astype(jnp.float32)
    key_scaled = keys_in.astype(jnp.float32) * head_dim ** (-0.5)
    value_wide = values_in.astype(jnp.float32)
    new_stabilizer = jnp.maximum(forget + stabilizer, ingate)
    retain = jnp.exp(forget + stabilizer - new_stabilizer)
    inflow = jnp.exp(ingate - new_stabilizer)
    new_memory = retain[..., None, None] * memory + (inflow[..., None] * value_wide)[..., :, None] * key_scaled[..., None, :]
    new_normalizer = retain[..., None] * normalizer + inflow[..., None] * key_scaled
    numerator = jnp.einsum('bhvk,bhk->bhv', new_memory, query_wide, precision=lax.Precision.HIGHEST)
    denominator = lax.optimization_barrier(jnp.sum(new_normalizer * query_wide, axis=-1))
    readout = numerator / jnp.maximum(jnp.abs(denominator), jnp.exp(-new_stabilizer))[..., None]
    centered = readout - lax.optimization_barrier(jnp.mean(readout, axis=-1, keepdims=True))
    normed = centered * lax.rsqrt(lax.optimization_barrier(jnp.mean(centered * centered, axis=-1, keepdims=True)) + epsilon)
    gated_out = normed * head_scale.astype(jnp.float32) * jax.nn.sigmoid(outgates.astype(jnp.float32))
    return (gated_out.astype(jnp.bfloat16), new_memory, new_normalizer, new_stabilizer)

def reference(tokens, gain_mixer, weight_query, weight_key, weight_value, weight_outgate, weight_ingate, weight_forget, bias_input, bias_forget, memory, normalizer, stabilizer, head_gain, weight_out, gain_channel, weight_up, weight_down):
    tokens_wide = tokens.astype(jnp.float32)
    scaled = (tokens_wide * gain_mixer.astype(jnp.float32)).astype(jnp.bfloat16)
    inverse = lax.rsqrt(lax.optimization_barrier(jnp.mean(tokens_wide * tokens_wide, axis=1)) + epsilon)[:, None]
    head_shape = (BATCH, HEADS, HD)
    queries = (inverse * project(scaled, weight_query)).astype(jnp.bfloat16).reshape(head_shape)
    keys_proj = (inverse * project(scaled, weight_key)).astype(jnp.bfloat16).reshape(head_shape)
    values_proj = (inverse * project(scaled, weight_value)).astype(jnp.bfloat16).reshape(head_shape)
    outgates = (inverse * project(scaled, weight_outgate)).astype(jnp.bfloat16).reshape(head_shape)
    ingate = inverse * jnp.dot(scaled, weight_ingate, preferred_element_type=jnp.float32) + bias_input
    forget = jax.nn.log_sigmoid(inverse * jnp.dot(scaled, weight_forget, preferred_element_type=jnp.float32) + bias_forget)
    row_blocks = N_DP * N_KV

    def block_cell(blocked):
        return cell_update(*blocked, head_gain)
    blocked = tuple((array.reshape((row_blocks, SEQ_DEV) + array.shape[1:]) for array in (queries, keys_proj, values_proj, outgates, ingate, forget, memory, normalizer, stabilizer)))
    results = lax.map(block_cell, blocked)
    heads_out, new_memory, new_normalizer, new_stabilizer = tuple((array.reshape((BATCH,) + array.shape[2:]) for array in results))
    heads_flat = heads_out.reshape(BATCH, WIDTH)
    half_width = WIDTH // N_TP
    mixed_rows = tokens_wide
    for member in range(N_TP):
        partial_value = jnp.dot(heads_flat[:, member * half_width:(member + 1) * half_width], weight_out[member * half_width:(member + 1) * half_width], preferred_element_type=jnp.float32).astype(jnp.bfloat16)
        mixed_rows = mixed_rows + partial_value.astype(jnp.float32)
    mixed_rows = mixed_rows.astype(jnp.bfloat16)
    mixed_wide = mixed_rows.astype(jnp.float32)
    scaled_mlp = (mixed_wide * gain_channel.astype(jnp.float32)).astype(jnp.bfloat16)
    inverse_mlp = lax.rsqrt(lax.optimization_barrier(jnp.mean(mixed_wide * mixed_wide, axis=1)) + epsilon)[:, None]
    activation = jax.nn.relu(inverse_mlp * jnp.dot(scaled_mlp, weight_up, preferred_element_type=jnp.float32))
    squared = (activation * activation).astype(jnp.bfloat16)
    layer_out = (mixed_wide + jnp.dot(squared, weight_down, preferred_element_type=jnp.float32)).astype(jnp.bfloat16)
    return (layer_out, new_memory, new_normalizer, new_stabilizer)
```

```python
import jax
import jax.numpy as jnp
from jax import lax
from jax.sharding import PartitionSpec as P

epsilon = 1e-06


def steps_of(size):
    if size & (size - 1) == 0:
        return [(k, [(i, i ^ k) for i in range(size)]) for k in range(size - 1, 0, -1)]
    return [(k, [(i, (i + k) % size) for i in range(size)]) for k in range(1, size)]


def peer_of(rank, step, size):
    return rank ^ step if size & (size - 1) == 0 else (rank + step) % size


def source_of(rank, step, size):
    return rank ^ step if size & (size - 1) == 0 else (rank - step) % size


def reduce_over(chunks, axis, size, rank):
    total = lax.dynamic_index_in_dim(chunks, rank, 0, keepdims=False).astype(jnp.float32)
    for step, pairs in steps_of(size):
        sent = lax.dynamic_index_in_dim(chunks, peer_of(rank, step, size), 0, keepdims=False)
        total = total + lax.ppermute(sent, axis, pairs).astype(jnp.float32)
    return total


def gather_over(piece, axis, size, rank):
    whole = jnp.zeros((size,) + piece.shape, piece.dtype)
    whole = lax.dynamic_update_index_in_dim(whole, piece, rank, 0)
    for step, pairs in steps_of(size):
        got = lax.ppermute(piece, axis, pairs)
        whole = lax.dynamic_update_index_in_dim(whole, got, source_of(rank, step, size), 0)
    return whole


def project(scaled, weight):
    return jnp.dot(scaled, weight.reshape(weight.shape[0], -1), preferred_element_type=jnp.float32)


def scale_slab(slab_rows, gain_slice):
    rows_wide = slab_rows.astype(jnp.float32)
    return (
        (rows_wide * gain_slice.astype(jnp.float32)).astype(jnp.bfloat16),
        jnp.sum(rows_wide * rows_wide, axis=1),
    )


def cell_update(
    queries, keys_in, values_in, outgates, ingate, forget, memory, normalizer, stabilizer, head_scale
):
    head_dim = queries.shape[-1]
    query_wide = queries.astype(jnp.float32)
    key_scaled = keys_in.astype(jnp.float32) * head_dim ** (-0.5)
    value_wide = values_in.astype(jnp.float32)
    new_stabilizer = jnp.maximum(forget + stabilizer, ingate)
    retain = jnp.exp(forget + stabilizer - new_stabilizer)
    inflow = jnp.exp(ingate - new_stabilizer)
    new_memory = (
        retain[..., None, None] * memory
        + (inflow[..., None] * value_wide)[..., :, None] * key_scaled[..., None, :]
    )
    new_normalizer = retain[..., None] * normalizer + inflow[..., None] * key_scaled
    numerator = jnp.einsum("bhvk,bhk->bhv", new_memory, query_wide, precision=lax.Precision.HIGHEST)
    denominator = jnp.sum(new_normalizer * query_wide, axis=-1)
    readout = numerator / jnp.maximum(jnp.abs(denominator), jnp.exp(-new_stabilizer))[..., None]
    centered = readout - jnp.mean(readout, axis=-1, keepdims=True)
    normed = centered * lax.rsqrt(jnp.mean(centered * centered, axis=-1, keepdims=True) + epsilon)
    gated_out = (
        normed * head_scale.astype(jnp.float32) * jax.nn.sigmoid(outgates.astype(jnp.float32))
    )
    return (gated_out.astype(jnp.bfloat16), new_memory, new_normalizer, new_stabilizer)


def solution(mesh):
    n_kv = mesh.shape["kv"]
    n_tp = mesh.shape["tp"]

    def body(
        tokens,
        gain_mixer,
        weight_query,
        weight_key,
        weight_value,
        weight_outgate,
        weight_ingate,
        weight_forget,
        bias_input,
        bias_forget,
        memory,
        normalizer,
        stabilizer,
        head_gain,
        weight_out,
        gain_channel,
        weight_up,
        weight_down,
    ):
        kv_rank = lax.axis_index("kv")
        tp_rank = lax.axis_index("tp")
        own_rows, heads_here, head_dim = memory.shape[:3]
        rows, own_cols = tokens.shape
        width_full = gain_mixer.shape[0]
        wide = heads_here * head_dim
        head_start = tp_rank * heads_here
        slab_cols = own_cols * n_tp
        col_start = kv_rank * slab_cols
        slab = gather_over(tokens, "tp", n_tp, tp_rank)
        slab_rows = slab.transpose(1, 0, 2).reshape(rows, slab_cols)
        scaled, squares = scale_slab(
            slab_rows, lax.dynamic_slice_in_dim(gain_mixer, col_start, slab_cols, 0)
        )
        gate_weights = jnp.concatenate(
            [
                lax.dynamic_slice(weight_ingate, (col_start, head_start), (slab_cols, heads_here)),
                lax.dynamic_slice(weight_forget, (col_start, head_start), (slab_cols, heads_here)),
            ],
            axis=1,
        )
        gate_part = jnp.dot(scaled, gate_weights, preferred_element_type=jnp.float32)
        extra = jnp.concatenate(
            [gate_part, squares[:, None], jnp.zeros((rows, 127 - 2 * heads_here), jnp.float32)], axis=1
        )
        partials = [
            project(scaled, weight).astype(jnp.bfloat16)
            for weight in (weight_query, weight_key, weight_value, weight_outgate)
        ] + [extra.astype(jnp.bfloat16)]
        chunks = jnp.concatenate(partials, axis=1).reshape(n_kv, own_rows, -1)
        summed = reduce_over(chunks, "kv", n_kv, kv_rank)
        extra = summed[:, 4 * wide :]
        inverse = lax.rsqrt(extra[:, 2 * heads_here] / width_full + epsilon)[:, None]
        head_view = (own_rows, heads_here, head_dim)
        queries, keys_proj, values_proj, outgates = (
            (inverse * summed[:, j * wide : (j + 1) * wide]).astype(jnp.bfloat16).reshape(head_view)
            for j in range(4)
        )
        gate_pre = inverse * extra[:, : 2 * heads_here]
        ingate = gate_pre[:, :heads_here] + lax.dynamic_slice_in_dim(
            bias_input, head_start, heads_here, 0
        )
        forget = jax.nn.log_sigmoid(
            gate_pre[:, heads_here:]
            + lax.dynamic_slice_in_dim(bias_forget, head_start, heads_here, 0)
        )
        head_scale = lax.dynamic_slice_in_dim(head_gain, head_start, heads_here, 0)
        heads_out, new_memory, new_normalizer, new_stabilizer = cell_update(
            queries,
            keys_proj,
            values_proj,
            outgates,
            ingate,
            forget,
            memory,
            normalizer,
            stabilizer,
            head_scale,
        )
        heads_flat = gather_over(heads_out.reshape(own_rows, wide), "kv", n_kv, kv_rank)
        partial_out = jnp.dot(
            heads_flat.reshape(rows, wide), weight_out, preferred_element_type=jnp.float32
        ).astype(jnp.bfloat16)
        both = gather_over(partial_out, "tp", n_tp, tp_rank)
        mixed_slab = (
            slab_rows.astype(jnp.float32) + jnp.sum(both.astype(jnp.float32), axis=0)
        ).astype(jnp.bfloat16)
        mixed = gather_over(mixed_slab, "kv", n_kv, kv_rank)
        mixed_rows = mixed.transpose(1, 0, 2).reshape(rows, width_full)
        scaled_mlp, squares_mlp = scale_slab(mixed_rows, gain_channel)
        up_total = jnp.dot(scaled_mlp, weight_up, preferred_element_type=jnp.float32)
        inverse_mlp = lax.rsqrt(squares_mlp / width_full + epsilon)[:, None]
        activation = jax.nn.relu(inverse_mlp * up_total)
        squared = (activation * activation).astype(jnp.bfloat16)
        down = jnp.dot(squared, weight_down, preferred_element_type=jnp.float32)
        down = down.reshape(rows, n_kv, n_tp, own_cols).transpose(2, 1, 0, 3)
        here = reduce_over(down.astype(jnp.bfloat16), "tp", n_tp, tp_rank)
        here = reduce_over(here.astype(jnp.bfloat16), "kv", n_kv, kv_rank)
        mixed_own = lax.dynamic_slice_in_dim(mixed_slab, tp_rank * own_cols, own_cols, 1)
        layer_out = (mixed_own.astype(jnp.float32) + here).astype(jnp.bfloat16)
        return (layer_out, new_memory, new_normalizer, new_stabilizer)

    placed = (
        P("dp", ("kv", "tp")),
        P(),
        P("kv", "tp", None),
        P("kv", "tp", None),
        P("kv", "tp", None),
        P("kv", "tp", None),
        P(),
        P(),
        P(),
        P(),
        P(("dp", "kv"), "tp", None, None),
        P(("dp", "kv"), "tp", None),
        P(("dp", "kv"), "tp"),
        P(),
        P("tp", "kv"),
        P(),
        P(None, ("kv", "tp")),
        P(("kv", "tp"), None),
    )
    return jax.shard_map(
        body,
        mesh=mesh,
        in_specs=placed,
        out_specs=(
            P("dp", ("kv", "tp")),
            P(("dp", "kv"), "tp", None, None),
            P(("dp", "kv"), "tp", None),
            P(("dp", "kv"), "tp"),
        ),
        check_vma=False,
    )
```

```python
import jax
import jax.numpy as jnp
from jax import lax
from jax.experimental import pallas as pl
from jax.experimental.pallas import tpu as pltpu
from jax.sharding import PartitionSpec as P

epsilon = 1e-06


def steps_of(size):
    if size & (size - 1) == 0:
        return [(k, [(i, i ^ k) for i in range(size)]) for k in range(size - 1, 0, -1)]
    return [(k, [(i, (i + k) % size) for i in range(size)]) for k in range(1, size)]


def peer_of(rank, step, size):
    return rank ^ step if size & (size - 1) == 0 else (rank + step) % size


def source_of(rank, step, size):
    return rank ^ step if size & (size - 1) == 0 else (rank - step) % size


def reduce_over(chunks, axis, size, rank):
    total = lax.dynamic_index_in_dim(chunks, rank, 0, keepdims=False).astype(jnp.float32)
    for step, pairs in steps_of(size):
        sent = lax.dynamic_index_in_dim(chunks, peer_of(rank, step, size), 0, keepdims=False)
        total = total + lax.ppermute(sent, axis, pairs).astype(jnp.float32)
    return total


def gather_over(piece, axis, size, rank):
    whole = jnp.zeros((size,) + piece.shape, piece.dtype)
    whole = lax.dynamic_update_index_in_dim(whole, piece, rank, 0)
    for step, pairs in steps_of(size):
        got = lax.ppermute(piece, axis, pairs)
        whole = lax.dynamic_update_index_in_dim(whole, got, source_of(rank, step, size), 0)
    return whole


def project(scaled, weight):
    return jnp.dot(scaled, weight.reshape(weight.shape[0], -1), preferred_element_type=jnp.float32)


def scale_slab(slab_rows, gain_slice):
    rows_wide = slab_rows.astype(jnp.float32)
    return (
        (rows_wide * gain_slice.astype(jnp.float32)).astype(jnp.bfloat16),
        jnp.sum(rows_wide * rows_wide, axis=1),
    )


def cell_update(
    queries, keys_in, values_in, outgates, ingate, forget, memory, normalizer, stabilizer, head_scale
):
    head_dim = queries.shape[-1]
    query_wide = queries.astype(jnp.float32)
    key_scaled = keys_in.astype(jnp.float32) * head_dim ** (-0.5)
    value_wide = values_in.astype(jnp.float32)
    new_stabilizer = jnp.maximum(forget + stabilizer, ingate)
    retain = jnp.exp(forget + stabilizer - new_stabilizer)
    inflow = jnp.exp(ingate - new_stabilizer)
    new_memory = (
        retain[..., None, None] * memory
        + (inflow[..., None] * value_wide)[..., :, None] * key_scaled[..., None, :]
    )
    new_normalizer = retain[..., None] * normalizer + inflow[..., None] * key_scaled
    numerator = jnp.einsum("bhvk,bhk->bhv", new_memory, query_wide, precision=lax.Precision.HIGHEST)
    denominator = jnp.sum(new_normalizer * query_wide, axis=-1)
    readout = numerator / jnp.maximum(jnp.abs(denominator), jnp.exp(-new_stabilizer))[..., None]
    centered = readout - jnp.mean(readout, axis=-1, keepdims=True)
    normed = centered * lax.rsqrt(jnp.mean(centered * centered, axis=-1, keepdims=True) + epsilon)
    gated_out = (
        normed * head_scale.astype(jnp.float32) * jax.nn.sigmoid(outgates.astype(jnp.float32))
    )
    return (gated_out.astype(jnp.bfloat16), new_memory, new_normalizer, new_stabilizer)


MIB = 1024 * 1024
VMEM = pl.BlockSpec(memory_space=pltpu.VMEM)
SMEM = pl.BlockSpec(memory_space=pltpu.SMEM)
WIDE = jnp.float32
NARROW = jnp.bfloat16


def shaped(shape, dtype):
    return jax.ShapeDtypeStruct(shape, dtype)


def kernel_call(ranks, kernel, name, outs, args, scratch=(), limit=8, cost_us=0, specs=None):
    single = not isinstance(outs, (list, tuple))
    cost = pl.CostEstimate(
        flops=int(cost_us * 1e9) + 1, bytes_accessed=int(cost_us * 3e6) + 1, transcendentals=0
    )
    return pl.pallas_call(
        kernel,
        out_shape=outs if single else tuple(outs),
        in_specs=[SMEM, SMEM] + (specs or [VMEM] * len(args)),
        out_specs=VMEM if single else (VMEM,) * len(outs),
        scratch_shapes=scratch,
        compiler_params=pltpu.CompilerParams(vmem_limit_bytes=limit * MIB),
        cost_estimate=cost,
        name=name,
    )(*ranks, *args)


def load_first(ranks, tokens, gain_tiles, in_rows, forget_rows, weights, heads_here, cols):
    parts = cols // 128
    count = 4 + len(weights)

    def kernel(kv_ref, tp_ref, tokens_ref, gain_ref, in_ref, forget_ref, *refs):
        weight_refs, outs, sems = refs[: len(weights)], refs[len(weights) : -1], refs[-1]
        mine_ref, own_gain_ref, gates_ref = outs[:3]
        tile = pl.multiple_of(kv_ref[0] * parts, 8)
        start = pl.multiple_of(kv_ref[0] * cols, 128)
        head = pl.multiple_of(tp_ref[0] * heads_here, 8)
        window = (pl.ds(head, heads_here), pl.ds(start, cols))
        pairs = [
            (tokens_ref, mine_ref),
            (gain_ref.at[pl.ds(tile, parts), :], own_gain_ref),
            (in_ref.at[window], gates_ref.at[pl.ds(0, heads_here), :]),
            (forget_ref.at[window], gates_ref.at[pl.ds(heads_here, heads_here), :]),
            *zip(weight_refs, outs[3:]),
        ]
        copies = [pltpu.make_async_copy(*pair, sems.at[n]) for n, pair in enumerate(pairs)]
        for copy in copies:
            copy.start()
        for copy in copies:
            copy.wait()

    args = (tokens, gain_tiles, in_rows, forget_rows, *weights)
    return kernel_call(
        ranks,
        kernel,
        "load_first",
        [
            shaped(tokens.shape, NARROW),
            shaped((parts, 128), NARROW),
            shaped((2 * heads_here, cols), NARROW),
        ]
        + [pltpu.VMEM(weight.shape, NARROW) for weight in weights],
        [pltpu.with_memory_space_constraint(arg, pltpu.HBM) for arg in args],
        scratch=[pltpu.SemaphoreType.DMA((count,))],
        cost_us=COST_LOAD,
        specs=[pl.BlockSpec(memory_space=pl.ANY)] * count,
    )


def start_block(ranks, mine, other, own_gain, gates):
    rows, own_cols = mine.shape
    cols = 2 * own_cols
    count = gates.shape[0]

    def kernel(kv_ref, tp_ref, mine_ref, other_ref, gain_ref, gates_ref, slab_ref, scaled_ref, extra_ref):
        first = tp_ref[0] == 0
        own = mine_ref[...].astype(WIDE)
        theirs = other_ref[...].astype(WIDE)
        gain = gain_ref[...].astype(WIDE)
        halves = (jnp.where(first, own, theirs), jnp.where(first, theirs, own))
        squares = jnp.zeros((rows, 1), WIDE)
        for half, slab in enumerate(halves):
            squares = squares + jnp.sum(slab * slab, axis=1, keepdims=True)
            slab_ref[:, half * own_cols : (half + 1) * own_cols] = slab.astype(NARROW)
            for part in range(own_cols // 128):
                tile = half * (own_cols // 128) + part
                scaled_ref[:, tile * 128 : (tile + 1) * 128] = (
                    slab[:, part * 128 : (part + 1) * 128] * gain[tile : tile + 1, :]
                ).astype(NARROW)
        extra_ref[...] = jnp.zeros(extra_ref.shape, WIDE)
        extra_ref[:, :count] = lax.dot_general(
            scaled_ref[...], gates_ref[...], (((1,), (1,)), ((), ())), preferred_element_type=WIDE
        )
        extra_ref[:, count : count + 1] = squares

    return kernel_call(
        ranks,
        kernel,
        "start_block",
        [shaped((rows, cols), NARROW), shaped((rows, cols), NARROW), shaped((rows, 128), WIDE)],
        (mine, other, own_gain, gates),
    )


def pack(ranks, partials, extra, n_kv):
    rows, wide = partials[0].shape
    own = rows // n_kv
    kinds = len(partials)
    steps = [step for step, _ in steps_of(n_kv)]
    shape = (kinds * own, wide + 128)

    def kernel(kv_ref, tp_ref, *refs):
        parts, extra_ref, outs, scratch = refs[:kinds], refs[kinds], refs[kinds + 1 : -1], refs[-1]
        scratch[:, :, wide:] = jnp.zeros((n_kv, kinds * own, 128), WIDE)
        for j in range(n_kv):
            for m in range(kinds):
                scratch[j, m * own : (m + 1) * own, :wide] = parts[m][j * own : (j + 1) * own, :]
            scratch[j, :own, wide:] = extra_ref[j * own : (j + 1) * own, :]
        outs[0][...] = scratch[kv_ref[0]]
        for out, step in zip(outs[1:], steps):
            out[...] = scratch[kv_ref[0] ^ step].astype(NARROW)

    return kernel_call(
        ranks,
        kernel,
        "pack",
        [shaped(shape, WIDE)] + [shaped(shape, NARROW)] * len(steps),
        (*partials, extra),
        scratch=[pltpu.VMEM((n_kv,) + shape, WIDE)],
        cost_us=COST_PACK,
    )


def cell(ranks, parts, bias_in, bias_forget, stabilizer, normalizer, head_gain, memory, width_full):
    own, heads, dim = normalizer.shape
    wide = heads * dim
    count = len(parts)

    def kernel(kv_ref, tp_ref, *refs):
        part_refs = refs[:count]
        (bias_in_ref, bias_forget_ref, stab_ref, norm_ref, gain_ref, memory_ref) = refs[count : count + 6]
        (heads_ref, new_norm_ref, new_stab_ref, retain_ref, values_ref, keys_ref, scratch) = refs[count + 6 :]
        total = part_refs[0][...]
        for ref in part_refs[1:]:
            total = total + ref[...].astype(WIDE)
        scratch[...] = total
        tp = tp_ref[0]
        inverse = lax.rsqrt(
            scratch[0:own, wide + 2 * heads : wide + 2 * heads + 1] / width_full + epsilon
        )

        def bias(ref):
            return jnp.where(tp == 0, ref[:, 0:heads], ref[:, heads : 2 * heads])

        ingate = inverse * scratch[0:own, wide : wide + heads] + bias(bias_in_ref)
        pre = inverse * scratch[0:own, wide + heads : wide + 2 * heads] + bias(bias_forget_ref)
        forget = jnp.minimum(pre, 0.0) - jnp.log1p(jnp.exp(-jnp.abs(pre)))
        carried = forget + stab_ref[...]
        new_stab = jnp.maximum(carried, ingate)
        retain = jnp.exp(carried - new_stab)
        inflow = jnp.exp(ingate - new_stab)
        floor = jnp.exp(-new_stab)
        new_stab_ref[...] = new_stab
        retain_ref[...] = retain
        gains = gain_ref[pl.ds(pl.multiple_of(tp * heads, 8), heads), :].astype(WIDE)
        which = lax.broadcasted_iota(jnp.int32, (own, dim), 0)
        for h in range(heads):
            lanes = slice(h * dim, (h + 1) * dim)
            query, key, value, gate = (
                (inverse * scratch[m * own : (m + 1) * own, lanes]).astype(NARROW) for m in range(4)
            )
            query_wide = query.astype(WIDE)
            key_scaled = key.astype(WIDE) * dim ** (-0.5)
            keep = retain[:, h : h + 1]
            value_in = inflow[:, h : h + 1] * value.astype(WIDE)
            keys_ref[:, h, :] = key_scaled
            values_ref[:, h, :] = value_in
            new_norm = keep * norm_ref[:, h, :] + inflow[:, h : h + 1] * key_scaled
            new_norm_ref[:, h, :] = new_norm
            denominator = jnp.sum(new_norm * query_wide, axis=1, keepdims=True)
            overlap = jnp.sum(key_scaled * query_wide, axis=1, keepdims=True)
            held = jnp.zeros((own, dim), WIDE)
            for b in range(own):
                block = memory_ref[b, h]
                high = block.astype(NARROW)
                low = (block - high.astype(WIDE)).astype(NARROW)
                dims = (((1,), (1,)), ((), ()))
                got = lax.dot_general(query, high, dims, preferred_element_type=WIDE)
                got = got + lax.dot_general(query, low, dims, preferred_element_type=WIDE)
                held = jnp.where(which == b, got, held)
            numerator = keep * held + value_in * overlap
            readout = numerator / jnp.maximum(jnp.abs(denominator), floor[:, h : h + 1])
            centered = readout - jnp.mean(readout, axis=1, keepdims=True)
            normed = centered * lax.rsqrt(jnp.mean(centered * centered, axis=1, keepdims=True) + epsilon)
            gated = normed * gains[h : h + 1, :] / (1.0 + jnp.exp(-gate.astype(WIDE)))
            heads_ref[:, lanes] = gated.astype(NARROW)

    return kernel_call(
        ranks,
        kernel,
        "cell",
        [
            shaped((own, wide), NARROW),
            shaped(normalizer.shape, WIDE),
            shaped(stabilizer.shape, WIDE),
            shaped(stabilizer.shape, WIDE),
            shaped(normalizer.shape, WIDE),
            shaped(normalizer.shape, WIDE),
        ],
        (*parts, bias_in, bias_forget, stabilizer, normalizer, head_gain, memory),
        scratch=[pltpu.VMEM(parts[0].shape, WIDE)],
        cost_us=COST_CELL,
    )


def out_step(ranks, own_heads, arrived, weight_out, later, n_kv):
    own, wide = own_heads.shape
    rows = own * n_kv
    steps = [step for step, _ in steps_of(n_kv)]

    def kernel(kv_ref, tp_ref, own_ref, *refs):
        got, weight_ref = refs[: len(steps)], refs[len(steps)]
        out_ref, stacked, flat = refs[-3:]
        kv = kv_ref[0]
        stacked[kv, :own, :] = own_ref[...].astype(WIDE)
        for ref, step in zip(got, steps):
            stacked[kv ^ step, :own, :] = ref[...].astype(WIDE)
        for j in range(n_kv):
            flat[j * own : (j + 1) * own, :] = stacked[j, :own, :]
        out_ref[...] = jnp.dot(
            flat[...].astype(NARROW), weight_ref[...], preferred_element_type=WIDE
        ).astype(NARROW)

    return kernel_call(
        ranks,
        kernel,
        "out_step",
        shaped((rows, weight_out.shape[1]), NARROW),
        (own_heads, *arrived, weight_out, *later),
        scratch=[pltpu.VMEM((n_kv, 8, wide), WIDE), pltpu.VMEM((rows, wide), WIDE)],
        cost_us=COST_OUT,
    )


def up_step(ranks, step, chunk, gain_tiles, weight_up, before):
    rows, cols = chunk.shape
    parts = cols // 128

    def kernel(kv_ref, tp_ref, chunk_ref, gain_ref, weight_ref, *refs):
        start = pl.multiple_of((kv_ref[0] ^ step) * cols, 128)
        wide = chunk_ref[...].astype(WIDE)
        tile = pl.multiple_of((kv_ref[0] ^ step) * parts, 8)
        gain = gain_ref[pl.ds(tile, parts), :].astype(WIDE)
        scaled = jnp.concatenate(
            [wide[:, p * 128 : (p + 1) * 128] * gain[p : p + 1, :] for p in range(parts)], axis=1
        ).astype(NARROW)
        part = jnp.dot(scaled, weight_ref[pl.ds(start, cols), :], preferred_element_type=WIDE)
        own = jnp.sum(wide * wide, axis=1, keepdims=True)
        if before:
            part = refs[0][...] + part
            own = refs[1][...] + own
        refs[-2][...] = part
        refs[-1][...] = own

    return kernel_call(
        ranks,
        kernel,
        "up_step",
        [shaped((rows, weight_up.shape[1]), WIDE), shaped((rows, 1), WIDE)],
        (chunk, gain_tiles, weight_up, *before),
        limit=4,
    )


def down_half(ranks, other, total, squares, weight_down, n_kv, width_full, dtype):
    rows = total.shape[0]
    cols = weight_down.shape[1] // (n_kv * 2)

    def kernel(kv_ref, tp_ref, total_ref, squares_ref, weight_ref, out_ref):
        inverse = lax.rsqrt(squares_ref[...] / width_full + epsilon)
        activation = jnp.maximum(inverse * total_ref[...], 0.0)
        squared = (activation * activation).astype(NARROW)
        half = tp_ref[0] ^ other
        for block in range(n_kv):
            start = pl.multiple_of((block * 2 + half) * cols, 128)
            out_ref[block] = jnp.dot(
                squared, weight_ref[:, pl.ds(start, cols)], preferred_element_type=WIDE
            ).astype(dtype)

    return kernel_call(
        ranks,
        kernel,
        "down_half",
        shaped((n_kv, rows, cols), dtype),
        (total, squares, weight_down),
        limit=4,
    )


def share(ranks, here, got, mixed_slab, n_kv):
    _, rows, cols = here.shape
    steps = [step for step, _ in steps_of(n_kv)]

    def kernel(kv_ref, tp_ref, here_ref, got_ref, mixed_ref, own_ref, *outs):
        kv = kv_ref[0]
        mixed = jnp.where(tp_ref[0] == 0, mixed_ref[:, :cols].astype(WIDE), mixed_ref[:, cols:].astype(WIDE))
        own_ref[...] = here_ref[kv] + got_ref[kv].astype(WIDE) + mixed
        for out, step in zip(outs, steps):
            out[...] = (here_ref[kv ^ step] + got_ref[kv ^ step].astype(WIDE)).astype(NARROW)

    return kernel_call(
        ranks,
        kernel,
        "share",
        [shaped((rows, cols), WIDE)] + [shaped((rows, cols), NARROW)] * len(steps),
        (here, got, mixed_slab),
    )


COST_LOAD = 0
COST_PACK = 40
COST_CELL = 0
COST_OUT = 0


def solution(mesh):
    n_kv = mesh.shape["kv"]
    n_tp = mesh.shape["tp"]

    def body(
        tokens,
        gain_mixer,
        weight_query,
        weight_key,
        weight_value,
        weight_outgate,
        weight_ingate,
        weight_forget,
        bias_input,
        bias_forget,
        memory,
        normalizer,
        stabilizer,
        head_gain,
        weight_out,
        gain_channel,
        weight_up,
        weight_down,
    ):
        kv_rank = lax.axis_index("kv")
        tp_rank = lax.axis_index("tp")
        own_rows, heads_here, head_dim = memory.shape[:3]
        rows, own_cols = tokens.shape
        width_full = gain_mixer.shape[0]
        wide = heads_here * head_dim
        head_start = tp_rank * heads_here
        slab_cols = own_cols * n_tp
        col_start = kv_rank * slab_cols
        slab = gather_over(tokens, "tp", n_tp, tp_rank)
        slab_rows = slab.transpose(1, 0, 2).reshape(rows, slab_cols)
        scaled, squares = scale_slab(
            slab_rows, lax.dynamic_slice_in_dim(gain_mixer, col_start, slab_cols, 0)
        )
        gate_weights = jnp.concatenate(
            [
                lax.dynamic_slice(weight_ingate, (col_start, head_start), (slab_cols, heads_here)),
                lax.dynamic_slice(weight_forget, (col_start, head_start), (slab_cols, heads_here)),
            ],
            axis=1,
        )
        gate_part = jnp.dot(scaled, gate_weights, preferred_element_type=jnp.float32)
        extra = jnp.concatenate(
            [gate_part, squares[:, None], jnp.zeros((rows, 127 - 2 * heads_here), jnp.float32)], axis=1
        )
        partials = [
            project(scaled, weight).astype(jnp.bfloat16)
            for weight in (weight_query, weight_key, weight_value, weight_outgate)
        ] + [extra.astype(jnp.bfloat16)]
        chunks = jnp.concatenate(partials, axis=1).reshape(n_kv, own_rows, -1)
        summed = reduce_over(chunks, "kv", n_kv, kv_rank)
        extra = summed[:, 4 * wide :]
        inverse = lax.rsqrt(extra[:, 2 * heads_here] / width_full + epsilon)[:, None]
        head_view = (own_rows, heads_here, head_dim)
        queries, keys_proj, values_proj, outgates = (
            (inverse * summed[:, j * wide : (j + 1) * wide]).astype(jnp.bfloat16).reshape(head_view)
            for j in range(4)
        )
        gate_pre = inverse * extra[:, : 2 * heads_here]
        ingate = gate_pre[:, :heads_here] + lax.dynamic_slice_in_dim(
            bias_input, head_start, heads_here, 0
        )
        forget = jax.nn.log_sigmoid(
            gate_pre[:, heads_here:]
            + lax.dynamic_slice_in_dim(bias_forget, head_start, heads_here, 0)
        )
        head_scale = lax.dynamic_slice_in_dim(head_gain, head_start, heads_here, 0)
        heads_out, new_memory, new_normalizer, new_stabilizer = cell_update(
            queries,
            keys_proj,
            values_proj,
            outgates,
            ingate,
            forget,
            memory,
            normalizer,
            stabilizer,
            head_scale,
        )
        heads_flat = gather_over(heads_out.reshape(own_rows, wide), "kv", n_kv, kv_rank)
        partial_out = jnp.dot(
            heads_flat.reshape(rows, wide), weight_out, preferred_element_type=jnp.float32
        ).astype(jnp.bfloat16)
        both = gather_over(partial_out, "tp", n_tp, tp_rank)
        mixed_slab = (
            slab_rows.astype(jnp.float32) + jnp.sum(both.astype(jnp.float32), axis=0)
        ).astype(jnp.bfloat16)
        mixed = gather_over(mixed_slab, "kv", n_kv, kv_rank)
        mixed_rows = mixed.transpose(1, 0, 2).reshape(rows, width_full)
        scaled_mlp, squares_mlp = scale_slab(mixed_rows, gain_channel)
        up_total = jnp.dot(scaled_mlp, weight_up, preferred_element_type=jnp.float32)
        inverse_mlp = lax.rsqrt(squares_mlp / width_full + epsilon)[:, None]
        activation = jax.nn.relu(inverse_mlp * up_total)
        squared = (activation * activation).astype(jnp.bfloat16)
        down = jnp.dot(squared, weight_down, preferred_element_type=jnp.float32)
        down = down.reshape(rows, n_kv, n_tp, own_cols).transpose(2, 1, 0, 3)
        here = reduce_over(down.astype(jnp.bfloat16), "tp", n_tp, tp_rank)
        here = reduce_over(here.astype(jnp.bfloat16), "kv", n_kv, kv_rank)
        mixed_own = lax.dynamic_slice_in_dim(mixed_slab, tp_rank * own_cols, own_cols, 1)
        layer_out = (mixed_own.astype(jnp.float32) + here).astype(jnp.bfloat16)
        return (layer_out, new_memory, new_normalizer, new_stabilizer)

    swap = [(0, 1), (1, 0)]

    def fast_body(
        tokens,
        gain_mixer,
        weight_query,
        weight_key,
        weight_value,
        weight_outgate,
        weight_ingate,
        weight_forget,
        bias_input,
        bias_forget,
        memory,
        normalizer,
        stabilizer,
        head_gain,
        weight_out,
        gain_channel,
        weight_up,
        weight_down,
    ):
        ranks = (lax.axis_index("kv").reshape(1), lax.axis_index("tp").reshape(1))
        heads_here = memory.shape[1]
        width_full = gain_mixer.shape[0]
        other = lax.ppermute(tokens, "tp", swap)
        mine, own_gain, gates, *weights = load_first(
            ranks,
            tokens,
            gain_mixer.reshape(-1, 128),
            weight_ingate.T,
            weight_forget.T,
            (weight_query, weight_key, weight_value, weight_outgate),
            heads_here,
            2 * tokens.shape[1],
        )
        slab, scaled, extra = start_block(ranks, mine, other, own_gain, gates)
        partials = [project(scaled, weight) for weight in weights]
        own, *sends = pack(ranks, partials, extra, n_kv)
        parts = [own] + [
            lax.ppermute(send, "kv", pairs) for send, (_, pairs) in zip(sends, steps_of(n_kv))
        ]
        heads_out, new_normalizer, new_stabilizer, retain, values_in, keys_scaled = cell(
            ranks,
            parts,
            bias_input.reshape(1, -1),
            bias_forget.reshape(1, -1),
            stabilizer,
            normalizer,
            head_gain,
            memory,
            width_full,
        )
        arrived = [lax.ppermute(heads_out, "kv", pairs) for _, pairs in steps_of(n_kv)]
        new_memory = (
            retain[..., None, None] * memory + values_in[..., :, None] * keys_scaled[..., None, :]
        )
        partial_out = out_step(
            ranks, heads_out, arrived, weight_out, (weight_up, weight_down), n_kv
        )
        partial_other = lax.ppermute(partial_out, "tp", swap)
        mixed_slab = (
            slab.astype(jnp.float32)
            + (partial_out.astype(jnp.float32) + partial_other.astype(jnp.float32))
        ).astype(jnp.bfloat16)
        chunks = [(0, mixed_slab)] + [
            (step, lax.ppermute(mixed_slab, "kv", pairs)) for step, pairs in steps_of(n_kv)
        ]
        before = ()
        for step, chunk in chunks:
            before = up_step(ranks, step, chunk, gain_channel.reshape(-1, 128), weight_up, before)
        theirs = down_half(ranks, 1, *before, weight_down, n_kv, width_full, jnp.bfloat16)
        got = lax.ppermute(theirs, "tp", swap)
        here = down_half(ranks, 0, *before, weight_down, n_kv, width_full, jnp.float32)
        own, *sends = share(ranks, here, got, mixed_slab, n_kv)
        for send, (_, pairs) in zip(sends, steps_of(n_kv)):
            own = own + lax.ppermute(send, "kv", pairs).astype(jnp.float32)
        return (own.astype(jnp.bfloat16), new_memory, new_normalizer, new_stabilizer)

    def chosen(tokens, *rest):
        memory = rest[9]
        fits = (
            n_tp == 2
            and n_kv in (2, 4, 8)
            and tokens.shape[1] % 512 == 0
            and memory.shape[0] <= 8
            and memory.shape[1] == 8
            and memory.shape[2] == 128
        )
        return (fast_body if fits else body)(tokens, *rest)

    placed = (
        P("dp", ("kv", "tp")),
        P(),
        P("kv", "tp", None),
        P("kv", "tp", None),
        P("kv", "tp", None),
        P("kv", "tp", None),
        P(),
        P(),
        P(),
        P(),
        P(("dp", "kv"), "tp", None, None),
        P(("dp", "kv"), "tp", None),
        P(("dp", "kv"), "tp"),
        P(),
        P("tp", "kv"),
        P(),
        P(None, ("kv", "tp")),
        P(("kv", "tp"), None),
    )
    return jax.shard_map(
        chosen,
        mesh=mesh,
        in_specs=placed,
        out_specs=(
            P("dp", ("kv", "tp")),
            P(("dp", "kv"), "tp", None, None),
            P(("dp", "kv"), "tp", None),
            P(("dp", "kv"), "tp"),
        ),
        check_vma=False,
    )
```
